32 devices in a mesh: sp: 8 (over z, y), tp: 4 (over x, core).
Axes of the slice: x: 2, y: 2, z: 4, core: 2. Of those that a mesh axis runs over, the one named last changes fastest.
Arguments:
- residual: bfloat16 [8192, 2048], P(('sp', 'tp')), may hold values from -6 to 6
- pool_input: bfloat16 [8192, 1024], P('sp', 'tp'), may hold values from -6 to 6
- doc_ids: int32 [8192], P('sp'), may hold values from 0 to 3, never falling along the last dimension, each value on 1 to 4096 neighbouring positions
- pool_map: bfloat16 [4, 256, 256], P('tp'), may hold values from -0.375 to 0.375
- pool_scale: float32 [1024], P('tp'), may hold values from 0.1 to 1.9
- out_weight: bfloat16 [1024, 2048], replicated, may hold values from -0.1875 to 0.1875
- mix_gain: float32 [2048], replicated, may hold values from 0.1 to 1.9
- mix_shift: float32 [2048], replicated, may hold values from -1.75 to 1.75
- group_router: bfloat16 [2048, 4], replicated, may hold values from -0.125 to 0.125
- expert_router: bfloat16 [2048, 8], replicated, may hold values from -0.125 to 0.125
- expert_gate: bfloat16 [8, 2048, 512], P('sp'), may hold values from -0.375 to 0.375
- expert_up: bfloat16 [8, 2048, 512], P('sp'), may hold values from -0.375 to 0.375
- expert_down: bfloat16 [8, 512, 2048], P('sp'), may hold values from -0.75 to 0.75
- routes: int32 [8192, 2], P(('sp', 'tp')), may hold values from 0 to 7, as said below
- ffn_gain: float32 [2048], replicated, may hold values from 0.1 to 1.9
- ffn_shift: float32 [2048], replicated, may hold values from -1.75 to 1.75
Outputs:
- layer_out: bfloat16 [8192, 2048], P(('sp', 'tp'))
The draws below stay inside these ranges and needn't reach their ends.
Inputs may be any that keep to these rules, and one draw needn't show every extreme that they name: `doc_ids`: document numbers never fall along the positions; each document has 1 to 4096 positions. `routes`: A token names 2 different experts. In each aligned block of half of one device's 256 rows, 4 experts are named exactly 64 times each and the others not at all.
All inputs are finite; a program needn't handle non-finite values.
Results may differ from the reference program's by a relative error of at most 0.0073.
Values may be sent and summed in bfloat16 or wider, within the bound.
A program may use at most 128 MiB of HBM per device.

```python
import math
import jax
import jax.numpy as jnp
import numpy as np
from jax import lax

D = 2048
POOL = 1024
PGROUPS = 4
GW = 256
FF = 512
MGROUPS = 4
TOPK = 2
SEQ_DEV = 1024
ROWS = 256
TOKENS = 8192
EXPERTS = 8
SLOTS = 64
N_SP = 8


def draw_routes(key, part):
    block_rows = ROWS // 2
    block_count = TOKENS // block_rows
    named_count = EXPERTS // 2
    anchor = jax.random.randint(jax.random.fold_in(key, 7), (), 0, EXPERTS).astype(jnp.int32)
    block_seeds = jax.random.split(jax.random.fold_in(key, 11), block_count)

    def one_block(block_seed):
        seeds = jax.random.split(block_seed, TOPK + 2)
        others = (anchor + 1 + jax.random.permutation(seeds[0], EXPERTS - 1).astype(jnp.int32)) % EXPERTS
        chosen = jnp.concatenate([anchor[None], others[:named_count - 1]]).astype(jnp.int32)
        listed = chosen[jnp.arange(named_count * SLOTS, dtype=jnp.int32) // SLOTS]
        columns = []
        for column in range(TOPK):
            segment = listed[column * block_rows:(column + 1) * block_rows]
            order = jax.random.permutation(seeds[column + 1], block_rows).astype(jnp.int32)
            columns.append(segment[order])
        table = jnp.stack(columns, axis=1)
        rotation = jax.random.randint(seeds[TOPK + 1], (block_rows,), 0, TOPK).astype(jnp.int32)
        column_index = (jnp.arange(TOPK, dtype=jnp.int32)[None, :] + rotation[:, None]) % TOPK
        return jnp.take_along_axis(table, column_index, axis=1)
    blocks = jax.vmap(one_block)(block_seeds)
    return blocks.reshape(TOKENS, TOPK).astype(jnp.int32)


def level_of(stream_key, shape, shards, low, high):
    level, own = 1.0, jax.random.fold_in(stream_key, 6)
    for position, shards_of in shards:
        steps = jnp.exp(jax.random.uniform(jax.random.fold_in(own, position), (shards_of,), jnp.float32, low / len(shards), high / len(shards)))
        level = level * jnp.repeat(steps, shape[position] // shards_of).reshape([-1 if axis == position else 1 for axis in range(len(shape))])
    return level


def length_profile(amount, total, bound, lean):
    portions = [(1 << 20) // math.isqrt(rank ** lean) + 1 for rank in range(2, amount + 1)]
    spare, given = total - bound - (amount - 1), [1] * (amount - 1)
    while spare > 0:
        free = [i for i in range(amount - 1) if given[i] < bound]
        pool, remaining = sum([portions[i] for i in free]), spare
        for i in free:
            extra = min(bound - given[i], max(1, remaining * portions[i] // pool), spare)
            given[i] = given[i] + extra
            spare = spare - extra
    return np.array([bound] + given)


def uneven(stream_key, number_of, total, limit, slope):
    if number_of == 2:
        one = jax.random.randint(stream_key, (), max(1, total - limit), min(limit, total - 1) + 1)
        return jnp.stack([one, total - one])
    tallies = jnp.asarray(length_profile(number_of, total, limit, slope), jnp.int32)
    couples = (number_of - 1) // 2
    source_of, taker = tallies[1:1 + 2 * couples:2], tallies[2:2 + 2 * couples:2]
    slack = jnp.minimum(source_of - 1, limit - taker)
    moved = jax.random.randint(jax.random.fold_in(stream_key, 1), (couples,), 0, 1 << 20) % (slack + 1)
    tallies = tallies.at[1:1 + 2 * couples:2].set(source_of - moved).at[2:2 + 2 * couples:2].set(taker + moved)
    return tallies[jax.random.permutation(jax.random.fold_in(stream_key, 2), number_of)]


def bell_draw(rng, dims, width, reach, cuts=(), kind=jnp.bfloat16):
    values = jax.random.normal(rng, dims, jnp.float32) * width
    if len(cuts) > 0:
        values = level_of(rng, dims, cuts, -0.22, 0.18) * values
    return jnp.clip(values, min=-reach, max=reach).astype(kind)


def setup_inputs(seed: int = 0) -> dict:
    key_list = jax.random.split(jax.random.key(seed), 17)
    residual = bell_draw(key_list[0], (TOKENS, D), 1.0, 6.0, ((0, 32),))
    pool_input = bell_draw(key_list[1], (TOKENS, POOL), 1.0, 6.0, ((0, 8), (1, 4)))
    doc_ids = jnp.searchsorted(jnp.cumsum(uneven(key_list[2], N_SP // 2, TOKENS, 4 * SEQ_DEV, 1)), jnp.arange(TOKENS), side="right").astype(jnp.int32)
    pool_map = bell_draw(key_list[3], (PGROUPS, GW, GW), GW ** -0.5, 0.375, ((0, 4),))
    pool_scale = jnp.clip(1.0 + 0.18 * jax.random.normal(key_list[4], (POOL,), jnp.float32), 0.1, 1.9)
    out_weight = bell_draw(key_list[5], (POOL, D), POOL ** -0.5, 0.1875)
    mix_gain = jnp.clip(1.0 + 0.18 * jax.random.normal(key_list[6], (D,), jnp.float32), 0.1, 1.9)
    mix_shift = bell_draw(key_list[7], (D,), 0.3, 1.75, (), jnp.float32)
    group_router = bell_draw(key_list[8], (D, MGROUPS), D ** -0.5, 0.125)
    expert_router = bell_draw(key_list[9], (D, EXPERTS), D ** -0.5, 0.125)
    expert_gate = bell_draw(key_list[10], (EXPERTS, D, FF), (D // 8) ** -0.5, 0.375, ((0, 8),))
    expert_up = bell_draw(key_list[11], (EXPERTS, D, FF), (D // 8) ** -0.5, 0.375, ((0, 8),))
    expert_down = bell_draw(key_list[12], (EXPERTS, FF, D), (FF // 8) ** -0.5, 0.75, ((0, 8),))
    routes = draw_routes(jax.random.fold_in(key_list[16], 71), 0)
    ffn_gain = jnp.clip(1.0 + 0.18 * jax.random.normal(key_list[14], (D,), jnp.float32), 0.1, 1.9)
    ffn_shift = bell_draw(key_list[15], (D,), 0.3, 1.75, (), jnp.float32)
    return {"residual": residual, "pool_input": pool_input, "doc_ids": doc_ids, "pool_map": pool_map, "pool_scale": pool_scale, "out_weight": out_weight, "mix_gain": mix_gain, "mix_shift": mix_shift, "group_router": group_router, "expert_router": expert_router, "expert_gate": expert_gate, "expert_up": expert_up, "expert_down": expert_down, "routes": routes, "ffn_gain": ffn_gain, "ffn_shift": ffn_shift}


skip_scale = 2.0 ** 0.5
epsilon = 1e-05

def layer_norm(values, norm_gain, norm_shift):
    center = values - lax.optimization_barrier(jnp.mean(values, axis=-1, keepdims=True))
    spread = lax.optimization_barrier(jnp.mean(center * center, axis=-1, keepdims=True))
    return center * lax.rsqrt(spread + epsilon) * norm_gain + norm_shift

def route_weights(normed, chosen, group_router, expert_router):
    group_logits = jnp.dot(normed, group_router, preferred_element_type=jnp.float32)
    expert_logits = jnp.dot(normed, expert_router, preferred_element_type=jnp.float32)
    group_count = group_logits.shape[1]
    expert_count = expert_logits.shape[1]
    group_exp = jnp.exp(group_logits)
    group_prob = group_exp / lax.optimization_barrier(jnp.sum(group_exp, axis=1, keepdims=True))
    expert_ids = jnp.arange(expert_count, dtype=jnp.int32)
    picked = lax.optimization_barrier(jnp.sum(jnp.where(chosen[:, :, None] == expert_ids[None, None, :], expert_logits[:, None, :], 0.0), axis=2))
    picked_exp = jnp.exp(picked)
    pair_share = picked_exp / lax.optimization_barrier(jnp.sum(picked_exp, axis=1, keepdims=True))
    group_of = chosen // (expert_count // group_count)
    group_ids = jnp.arange(group_count, dtype=jnp.int32)
    group_share = lax.optimization_barrier(jnp.sum(jnp.where(group_of[:, :, None] == group_ids[None, None, :], group_prob[:, None, :], 0.0), axis=2))
    return group_share * pair_share

def pool_group(values, doc_ids, window):
    length = values.shape[0]
    source = values.astype(jnp.float32)
    running = jnp.zeros_like(source)
    weight_sum = jnp.zeros((length, 1), jnp.float32)
    for offset in range(window):
        earlier = jnp.pad(source, ((offset, 0), (0, 0)))[:length]
        earlier_docs = jnp.pad(doc_ids, (offset, 0), constant_values=-1)[:length]
        same_doc = (earlier_docs == doc_ids).astype(jnp.float32)[:, None]
        running = running + same_doc * earlier
        weight_sum = weight_sum + same_doc
    return running / weight_sum - source

def expert_sum(normed, routes, weight, expert_gate, expert_up, expert_down):
    flat_routes = routes.reshape(-1).astype(jnp.int32)
    entry_count = flat_routes.shape[0]
    sorted_entries = jnp.argsort(flat_routes, stable=True).astype(jnp.int32)
    counts = lax.optimization_barrier(jnp.sum((flat_routes[:, None] == jnp.arange(EXPERTS, dtype=jnp.int32)[None, :]).astype(jnp.int32), axis=0))
    starts = (jnp.cumsum(counts) - counts).astype(jnp.int32)
    load_limit = TOKENS // (ROWS // 2) * SLOTS
    entries_padded = jnp.concatenate([sorted_entries, jnp.full((load_limit,), entry_count, jnp.int32)])
    flat_weight = jnp.concatenate([weight.reshape(-1), jnp.zeros((1,), jnp.float32)])
    padded_rows = jnp.concatenate([normed, jnp.zeros((1, normed.shape[1]), normed.dtype)], axis=0)

    def expert_step(routed_sum, expert):
        entry_ids = lax.dynamic_slice_in_dim(entries_padded, starts[expert], load_limit)
        live_mask = jnp.arange(load_limit, dtype=jnp.int32) < counts[expert]
        entry_ids = jnp.where(live_mask, entry_ids, entry_count).astype(jnp.int32)
        token_ids = (entry_ids // TOPK).astype(jnp.int32)
        gathered = padded_rows[token_ids]
        gate_out = jnp.dot(gathered, expert_gate[expert], preferred_element_type=jnp.float32)
        up_out = jnp.dot(gathered, expert_up[expert], preferred_element_type=jnp.float32)
        hidden = (jax.nn.silu(gate_out) * up_out).astype(jnp.bfloat16)
        result = jnp.dot(hidden, expert_down[expert], preferred_element_type=jnp.float32).astype(jnp.bfloat16)
        term = flat_weight[entry_ids][:, None] * result.astype(jnp.float32)
        return (routed_sum.at[token_ids].add(term), None)
    routed_sum = jnp.zeros((TOKENS + 1, normed.shape[1]), jnp.float32)
    routed_sum, unused = lax.scan(expert_step, routed_sum, jnp.arange(EXPERTS, dtype=jnp.int32))
    return routed_sum[:TOKENS]

def reference(residual, pool_input, doc_ids, pool_map, pool_scale, out_weight, mix_gain, mix_shift, group_router, expert_router, expert_gate, expert_up, expert_down, routes, ffn_gain, ffn_shift):
    mixed_parts = []
    for group_index in range(PGROUPS):
        columns = slice(group_index * GW, (group_index + 1) * GW)
        pooled = pool_group(pool_input[:, columns], doc_ids, 2 ** (group_index + 1)).astype(jnp.bfloat16)
        mapped = jnp.dot(pooled, pool_map[group_index], preferred_element_type=jnp.float32) * pool_scale[columns]
        mixed_parts.append(mapped.astype(jnp.bfloat16))
    mixed = jnp.concatenate(mixed_parts, axis=1)
    branch = jnp.dot(mixed, out_weight, preferred_element_type=jnp.float32)
    normed = layer_norm(skip_scale * residual.astype(jnp.float32) + branch, mix_gain, mix_shift).astype(jnp.bfloat16)
    weight = route_weights(normed, routes, group_router, expert_router)
    routed = expert_sum(normed, routes, weight, expert_gate, expert_up, expert_down)
    return layer_norm(skip_scale * normed.astype(jnp.float32) + routed, ffn_gain, ffn_shift).astype(jnp.bfloat16)
```

```python
import functools

import jax
import jax.numpy as jnp
from jax import lax
from jax.experimental import pallas as pl
from jax.experimental.pallas import tpu as pltpu
from jax.sharding import PartitionSpec as P

skip_scale = 2.0**0.5
epsilon = 1e-05


def from_behind(block, axis, distance):
    devices = range(lax.axis_size(axis))
    route = [(i - distance, i) for i in devices if i - distance in devices]
    return lax.ppermute(block, axis, route)


def layer_norm(values, norm_gain, norm_shift):
    center = values - jnp.mean(values, axis=-1, keepdims=True)
    spread = jnp.mean(center * center, axis=-1, keepdims=True)
    return center * lax.rsqrt(spread + epsilon) * norm_gain + norm_shift


def route_weights(normed, chosen, group_router, expert_router):
    group_logits = jnp.dot(normed, group_router, preferred_element_type=jnp.float32)
    expert_logits = jnp.dot(normed, expert_router, preferred_element_type=jnp.float32)
    group_count = group_logits.shape[1]
    expert_count = expert_logits.shape[1]
    group_exp = jnp.exp(group_logits)
    group_prob = group_exp / jnp.sum(group_exp, axis=1, keepdims=True)
    expert_ids = jnp.arange(expert_count, dtype=jnp.int32)
    picked = jnp.sum(
        jnp.where(chosen[:, :, None] == expert_ids[None, None, :], expert_logits[:, None, :], 0.0),
        axis=2,
    )
    picked_exp = jnp.exp(picked)
    pair_share = picked_exp / jnp.sum(picked_exp, axis=1, keepdims=True)
    group_of = chosen // (expert_count // group_count)
    group_ids = jnp.arange(group_count, dtype=jnp.int32)
    group_share = jnp.sum(
        jnp.where(group_of[:, :, None] == group_ids[None, None, :], group_prob[:, None, :], 0.0),
        axis=2,
    )
    return group_share * pair_share


def expert_ffn(arrived, expert_gate, expert_up, expert_down):
    sources, slot_count, width = arrived.shape
    gathered = arrived.reshape(sources * slot_count, width)
    gate_out = jnp.dot(gathered, expert_gate[0], preferred_element_type=jnp.float32)
    up_out = jnp.dot(gathered, expert_up[0], preferred_element_type=jnp.float32)
    hidden = (jax.nn.silu(gate_out) * up_out).astype(jnp.bfloat16)
    result = jnp.dot(hidden, expert_down[0], preferred_element_type=jnp.float32).astype(
        jnp.bfloat16
    )
    return result.reshape(sources, slot_count, width)


def fill_slots(normed, chosen, capacity, expert_count):
    flat_routes = chosen.reshape(-1)
    entry_count = flat_routes.shape[0]
    onehot = (flat_routes[:, None] == jnp.arange(expert_count, dtype=jnp.int32)[None, :]).astype(
        jnp.int32
    )
    slot_rank = jnp.sum((jnp.cumsum(onehot, axis=0) - onehot) * onehot, axis=1)
    slot_index = flat_routes * capacity + slot_rank
    token_ids = jnp.arange(entry_count, dtype=jnp.int32) // chosen.shape[1]
    source_row = (
        jnp.full((expert_count * capacity,), normed.shape[0], jnp.int32)
        .at[slot_index]
        .set(token_ids)
    )
    padded = jnp.concatenate([normed, jnp.zeros((1, normed.shape[1]), normed.dtype)], axis=0)
    outgoing = jnp.take(padded, source_row, axis=0).reshape(expert_count, capacity, normed.shape[1])
    return (outgoing, slot_index)


def combine_rows(returned, slot_index, weight):
    flat_out = returned.reshape(-1, returned.shape[2])
    picked = jnp.take(flat_out, slot_index, axis=0).reshape(
        weight.shape[0], weight.shape[1], flat_out.shape[1]
    )
    return jnp.sum(weight[:, :, None] * picked.astype(jnp.float32), axis=1)


MESH = pl.DeviceIdType.MESH
group_size = 4


def flip(index, bit):
    return index + bit - 2 * bit * ((index // bit) % 2)


def experts_kernel(
    dims,
    normed,
    meta,
    gate_piece,
    up_piece,
    own_gate,
    own_up,
    own_down,
    gain,
    shift,
    out,
    gate_a,
    up_a,
    down_a,
    gate_b,
    up_b,
    down_b,
    rows_in,
    meta_in,
    picked,
    spread,
    slot_weight,
    hidden,
    weighted,
    partial,
    passing,
    arrived,
    load_sems,
    send_sems,
    recv_sems,
):
    slots, expert_count = dims
    rows, width = normed.shape
    half = rows // 2
    ff = own_gate.shape[2]
    piece = gate_piece.shape[1]
    sp, tp = lax.axis_index("sp"), lax.axis_index("tp")
    to_y = {"sp": flip(sp, 1)}
    to_z = {"sp": flip(sp, 2)}
    to_far = {"sp": flip(sp, group_size)}
    to_x = {"tp": flip(tp, 2)}
    to_core = {"tp": flip(tp, 1)}

    loads = [
        pltpu.make_async_copy(own_gate.at[0], gate_a, load_sems.at[0]),
        pltpu.make_async_copy(own_up.at[0], up_a, load_sems.at[1]),
        pltpu.make_async_copy(own_down.at[0], down_a, load_sems.at[2]),
    ]
    for load in loads:
        load.start()

    barrier = pltpu.get_barrier_semaphore()
    peers = (to_y, to_z, to_far, to_x, to_core)
    for peer in peers:
        pl.semaphore_signal(barrier, inc=1, device_id=peer, device_id_type=MESH)
    pl.semaphore_wait(barrier, len(peers))

    made = []

    def send(src, dst, peer):
        index = len(made)
        copy = pltpu.make_async_remote_copy(
            src_ref=src,
            dst_ref=dst,
            send_sem=send_sems.at[index],
            recv_sem=recv_sems.at[index],
            device_id=peer,
            device_id_type=MESH,
        )
        copy.start()
        made.append(copy)
        return copy

    first, second = pl.ds(0, half), pl.ds(half, half)

    def cols(position):
        return pl.ds(pl.multiple_of(position * piece, piece), piece)

    mine, across, other, corner = cols(tp), cols(flip(tp, 2)), cols(flip(tp, 1)), None

    meta_y = send(meta, meta_in.at[0], to_y)
    meta_z = send(meta, meta_in.at[1], to_z)
    rows_y1 = send(normed.at[first], rows_in.at[0, first], to_y)
    rows_z2 = send(normed.at[second], rows_in.at[1, second], to_z)
    down_far = send(own_down.at[0, mine], down_b.at[mine], to_far)
    gate_x = send(gate_piece, gate_b.at[:, mine], to_x)
    up_x = send(up_piece, up_b.at[:, mine], to_x)
    gate_c = send(gate_piece, gate_b.at[:, mine], to_core)
    up_c = send(up_piece, up_b.at[:, mine], to_core)
    keep = [
        pltpu.make_async_copy(gate_piece, gate_b.at[:, mine], load_sems.at[3]),
        pltpu.make_async_copy(up_piece, up_b.at[:, mine], load_sems.at[4]),
    ]
    for load in keep:
        load.start()
    rows_y2 = send(normed.at[second], rows_in.at[0, second], to_y)
    rows_z1 = send(normed.at[first], rows_in.at[1, first], to_z)

    slot_ids = lax.broadcasted_iota(jnp.int32, (slots, rows), 0).astype(jnp.float32)
    experts = (sp, flip(sp, group_size))

    def select(position, row_ref, meta_ref):
        parts = []
        for which in range(2):
            slot_row = meta_ref[pl.ds(experts[which], 1), :]
            weight_row = meta_ref[pl.ds(expert_count + experts[which], 1), :]
            match = jnp.where(slot_ids == slot_row, 1.0, 0.0)
            slot_weight[position, pl.ds(which * slots, slots), :] = jnp.sum(
                match * weight_row, axis=1, keepdims=True
            )
            parts.append(match)
        match = jnp.concatenate(parts, axis=0)
        spread[position] = jnp.transpose(match).astype(jnp.bfloat16)
        match = match.astype(jnp.bfloat16)

        @pl.loop(0, 4)
        def _(step):
            wide = width // 4
            block = pl.ds(pl.multiple_of(step * wide, wide), wide)
            picked[position, :, block] = jnp.dot(
                match, row_ref[:, block], preferred_element_type=jnp.float32
            ).astype(jnp.bfloat16)

    def ffn(position, which, gate, up, down):
        where = pl.ds(which * slots, slots)

        @pl.loop(0, 2)
        def _(step):
            wide = ff // 2
            block = pl.ds(pl.multiple_of(step * wide, wide), wide)
            values = picked[position, where, :]
            gate_out = jnp.dot(values, gate[:, block], preferred_element_type=jnp.float32)
            up_out = jnp.dot(values, up[:, block], preferred_element_type=jnp.float32)
            hidden[:, block] = (gate_out / (1.0 + jnp.exp(-gate_out)) * up_out).astype(
                jnp.bfloat16
            )

        @pl.loop(0, 4)
        def _(step):
            wide = width // 4
            block = pl.ds(pl.multiple_of(step * wide, wide), wide)
            result = jnp.dot(hidden[...], down[:, block], preferred_element_type=jnp.float32)
            weighted[position, where, block] = (
                result * slot_weight[position, where, :]
            ).astype(jnp.bfloat16)

    def gather_back(position):
        @pl.loop(0, 4)
        def _(step):
            wide = width // 4
            block = pl.ds(pl.multiple_of(step * wide, wide), wide)
            partial[position, :, block] = jnp.dot(
                spread[position], weighted[position, :, block], preferred_element_type=jnp.float32
            ).astype(jnp.bfloat16)

    own, from_y, from_z, from_corner = 3, 0, 1, 2
    select(own, normed, meta)
    for load in loads:
        load.wait()
    ffn(own, 0, gate_a, up_a, down_a)

    meta_y.wait_recv()
    meta_corner = send(meta_in.at[0], meta_in.at[2], to_z)
    rows_y1.wait_recv()
    rows_corner1 = send(rows_in.at[0, first], rows_in.at[2, first], to_z)
    rows_z2.wait_recv()
    rows_corner2 = send(rows_in.at[1, second], rows_in.at[2, second], to_y)
    gate_x.wait_recv()
    gate_relay = send(gate_b.at[:, across], gate_b.at[:, across], to_core)
    up_x.wait_recv()
    up_relay = send(up_b.at[:, across], up_b.at[:, across], to_core)
    down_far.wait_recv()
    down_x = send(down_b.at[mine], down_b.at[mine], to_x)
    down_c = send(down_b.at[mine], down_b.at[mine], to_core)

    rows_y2.wait_recv()
    select(from_y, rows_in.at[0], meta_in.at[0])
    ffn(from_y, 0, gate_a, up_a, down_a)
    meta_z.wait_recv()
    rows_z1.wait_recv()
    select(from_z, rows_in.at[1], meta_in.at[1])
    ffn(from_z, 0, gate_a, up_a, down_a)
    down_x.wait_recv()
    down_relay = send(down_b.at[across], down_b.at[across], to_core)
    meta_corner.wait_recv()
    rows_corner1.wait_recv()
    rows_corner2.wait_recv()
    select(from_corner, rows_in.at[2], meta_in.at[2])
    ffn(from_corner, 0, gate_a, up_a, down_a)
    for load in keep:
        load.wait()
    for copy in (gate_c, up_c, gate_relay, up_relay, down_c, down_relay):
        copy.wait_recv()

    ffn(from_corner, 1, gate_b, up_b, down_b)
    gather_back(from_corner)
    pass_y = send(partial.at[from_corner, first], passing.at[0], to_y)
    pass_z = send(partial.at[from_corner, second], passing.at[1], to_z)
    ffn(from_y, 1, gate_b, up_b, down_b)
    gather_back(from_y)
    back_y1 = send(partial.at[from_y, first], arrived.at[0, first], to_y)
    ffn(from_z, 1, gate_b, up_b, down_b)
    gather_back(from_z)
    back_z2 = send(partial.at[from_z, second], arrived.at[1, second], to_z)

    def add_passing(position, where, slot):
        partial[position, where, :] = (
            partial[position, where, :].astype(jnp.float32) + passing[slot].astype(jnp.float32)
        ).astype(jnp.bfloat16)

    pass_y.wait_recv()
    add_passing(from_z, first, 0)
    back_z1 = send(partial.at[from_z, first], arrived.at[1, first], to_z)
    pass_z.wait_recv()
    add_passing(from_y, second, 1)
    back_y2 = send(partial.at[from_y, second], arrived.at[0, second], to_y)
    ffn(own, 1, gate_b, up_b, down_b)
    for copy in (back_y1, back_z2, back_z1, back_y2):
        copy.wait_recv()

    @pl.loop(0, rows // 64)
    def _(step):
        block = pl.ds(pl.multiple_of(step * 64, 64), 64)
        routed = jnp.dot(spread[own, block, :], weighted[own], preferred_element_type=jnp.float32)
        routed = routed + arrived[0, block, :].astype(jnp.float32)
        routed = routed + arrived[1, block, :].astype(jnp.float32)
        values = skip_scale * normed[block, :].astype(jnp.float32) + routed
        out[block, :] = layer_norm(values, gain[...], shift[...]).astype(jnp.bfloat16)

    for copy in made:
        copy.wait_send()


def routing_table(chosen, weight, expert_count, capacity):
    rows = chosen.shape[0]
    half = rows // 2
    onehot = (
        chosen[:, :, None] == jnp.arange(expert_count, dtype=jnp.int32)[None, None, :]
    ).astype(jnp.float32)
    named = jnp.sum(onehot, axis=1)
    before = jnp.tril(jnp.ones((half, half), jnp.bfloat16), -1)
    rank = jnp.einsum(
        "ab,hbe->hae",
        before,
        named.reshape(2, half, expert_count).astype(jnp.bfloat16),
        preferred_element_type=jnp.float32,
    )
    rank = rank + jnp.arange(2, dtype=jnp.float32)[:, None, None] * capacity
    slot = jnp.where(named > 0, rank.reshape(rows, expert_count), -1.0)
    share = jnp.sum(onehot * weight[:, :, None], axis=1)
    return jnp.concatenate([slot, share], axis=1).T


def near_experts(
    normed, weight, routes, pieces, expert_gate, expert_up, expert_down, ffn_gain, ffn_shift
):
    expert_count = lax.axis_size("sp")
    rows, width = normed.shape
    ff = expert_gate.shape[2]
    capacity = rows // 2 * routes.shape[1] * 2 // expert_count
    slots = 2 * capacity
    meta = routing_table(routes, weight, expert_count, capacity)
    vmem = pl.BlockSpec(memory_space=pltpu.VMEM)
    anywhere = pl.BlockSpec(memory_space=pl.ANY)
    bf16 = jnp.bfloat16
    return pl.pallas_call(
        functools.partial(experts_kernel, (slots, expert_count)),
        out_shape=jax.ShapeDtypeStruct((rows, width), bf16),
        in_specs=[vmem, vmem] + [anywhere] * 5 + [vmem, vmem],
        out_specs=vmem,
        scratch_shapes=[
            pltpu.VMEM((width, ff), bf16),
            pltpu.VMEM((width, ff), bf16),
            pltpu.VMEM((ff, width), bf16),
            pltpu.VMEM((width, ff), bf16),
            pltpu.VMEM((width, ff), bf16),
            pltpu.VMEM((ff, width), bf16),
            pltpu.VMEM((3, rows, width), bf16),
            pltpu.VMEM((3,) + meta.shape, jnp.float32),
            pltpu.VMEM((4, 2 * slots, width), bf16),
            pltpu.VMEM((4, rows, 2 * slots), bf16),
            pltpu.VMEM((4, 2 * slots, 1), jnp.float32),
            pltpu.VMEM((slots, ff), bf16),
            pltpu.VMEM((4, 2 * slots, width), bf16),
            pltpu.VMEM((3, rows, width), bf16),
            pltpu.VMEM((2, rows // 2, width), bf16),
            pltpu.VMEM((2, rows, width), bf16),
            pltpu.SemaphoreType.DMA((5,)),
            pltpu.SemaphoreType.DMA((25,)),
            pltpu.SemaphoreType.DMA((25,)),
        ],
        compiler_params=pltpu.CompilerParams(
            collective_id=0, has_side_effects=True, vmem_limit_bytes=60 * 1024 * 1024
        ),
    )(
        normed,
        meta,
        pieces[0],
        pieces[1],
        expert_gate,
        expert_up,
        expert_down,
        ffn_gain[None, :],
        ffn_shift[None, :],
    )


def on_device(
    residual,
    pool_input,
    doc_ids,
    pool_map,
    pool_scale,
    out_weight,
    mix_gain,
    mix_shift,
    group_router,
    expert_router,
    expert_gate,
    expert_up,
    expert_down,
    routes,
    ffn_gain,
    ffn_shift,
):
    seq_rows = pool_input.shape[0]
    reach_rows = 15
    expert_count = lax.axis_size("sp")
    tp_count = lax.axis_size("tp")
    near = expert_count == 2 * group_size and tp_count == group_size
    if near:
        piece = expert_gate.shape[2] // tp_count
        begin = lax.axis_index("tp") * piece
        swap = [(i, (i + group_size) % expert_count) for i in range(expert_count)]
        pieces = [
            lax.ppermute(lax.dynamic_slice_in_dim(part[0], begin, piece, axis=1), "sp", swap)
            for part in (expert_gate, expert_up)
        ]
    window = jnp.left_shift(jnp.int32(2), lax.axis_index("tp"))
    first_row = lax.axis_index("sp") * seq_rows
    tail_values, tail_docs = from_behind(
        (pool_input[seq_rows - reach_rows :], doc_ids[seq_rows - reach_rows :]), "sp", 1
    )
    source = jnp.concatenate([tail_values, pool_input], axis=0).astype(jnp.float32)
    all_docs = jnp.concatenate([tail_docs, doc_ids], axis=0)
    positions = first_row - reach_rows + jnp.arange(seq_rows + reach_rows, dtype=jnp.int32)
    running = jnp.zeros((seq_rows, source.shape[1]), jnp.float32)
    weight_sum = jnp.zeros((seq_rows, 1), jnp.float32)
    for offset in range(reach_rows + 1):
        begin_row = reach_rows - offset
        earlier = source[begin_row : begin_row + seq_rows]
        keep_mask = (
            (all_docs[begin_row : begin_row + seq_rows] == doc_ids)
            & (positions[begin_row : begin_row + seq_rows] >= 0)
            & (offset < window)
        )
        same_doc = keep_mask.astype(jnp.float32)[:, None]
        running = running + same_doc * earlier
        weight_sum = weight_sum + same_doc
    pooled = (running / weight_sum - source[reach_rows:]).astype(jnp.bfloat16)
    mixed = (jnp.dot(pooled, pool_map[0], preferred_element_type=jnp.float32) * pool_scale).astype(
        jnp.bfloat16
    )
    row_count = seq_rows // tp_count
    blocks = mixed.reshape(tp_count, row_count, mixed.shape[1])
    branch = jnp.einsum(
        "abc,cd->abd",
        lax.all_to_all(blocks, "tp", split_axis=0, concat_axis=2, tiled=True),
        out_weight,
        preferred_element_type=jnp.float32,
    )[0]
    normed = layer_norm(
        skip_scale * residual.astype(jnp.float32) + branch, mix_gain, mix_shift
    ).astype(jnp.bfloat16)
    weight = route_weights(normed, routes, group_router, expert_router)
    if near:
        return near_experts(
            normed, weight, routes, pieces, expert_gate, expert_up, expert_down, ffn_gain, ffn_shift
        )
    half_most = row_count * routes.shape[1] // expert_count
    half_rows = row_count // 2
    routed_parts = []
    for piece_index in range(2):
        rows_here = slice(piece_index * half_rows, (piece_index + 1) * half_rows)
        outgoing, slot_index = fill_slots(
            normed[rows_here], routes[rows_here], half_most, expert_count
        )
        returned = lax.all_to_all(
            expert_ffn(
                lax.all_to_all(outgoing, "sp", split_axis=0, concat_axis=0, tiled=True),
                expert_gate,
                expert_up,
                expert_down,
            ),
            "sp",
            split_axis=0,
            concat_axis=0,
            tiled=True,
        )
        routed_parts.append(combine_rows(returned, slot_index, weight[rows_here]))
    routed = jnp.concatenate(routed_parts, axis=0)
    return layer_norm(skip_scale * normed.astype(jnp.float32) + routed, ffn_gain, ffn_shift).astype(
        jnp.bfloat16
    )


def solution(mesh):
    in_specs = (
        P(("sp", "tp"), None),
        P("sp", "tp"),
        P("sp"),
        P("tp", None, None),
        P("tp"),
        P(),
        P(),
        P(),
        P(),
        P(),
        P("sp", None, None),
        P("sp", None, None),
        P("sp", None, None),
        P(("sp", "tp"), None),
        P(),
        P(),
    )
    out_specs = P(("sp", "tp"), None)
    return jax.shard_map(
        on_device, mesh=mesh, in_specs=in_specs, out_specs=out_specs, check_vma=False
    )
```

```python
import functools

import jax
import jax.numpy as jnp
from jax import lax
from jax.experimental import pallas as pl
from jax.experimental.pallas import tpu as pltpu
from jax.sharding import PartitionSpec as P

skip_scale = 2.0**0.5
epsilon = 1e-05


def from_behind(block, axis, distance):
    devices = range(lax.axis_size(axis))
    route = [(i - distance, i) for i in devices if i - distance in devices]
    return lax.ppermute(block, axis, route)


def layer_norm(values, norm_gain, norm_shift):
    center = values - jnp.mean(values, axis=-1, keepdims=True)
    spread = jnp.mean(center * center, axis=-1, keepdims=True)
    return center * lax.rsqrt(spread + epsilon) * norm_gain + norm_shift


def route_weights(normed, chosen, group_router, expert_router):
    group_logits = jnp.dot(normed, group_router, preferred_element_type=jnp.float32)
    expert_logits = jnp.dot(normed, expert_router, preferred_element_type=jnp.float32)
    group_count = group_logits.shape[1]
    expert_count = expert_logits.shape[1]
    group_exp = jnp.exp(group_logits)
    group_prob = group_exp / jnp.sum(group_exp, axis=1, keepdims=True)
    expert_ids = jnp.arange(expert_count, dtype=jnp.int32)
    picked = jnp.sum(
        jnp.where(chosen[:, :, None] == expert_ids[None, None, :], expert_logits[:, None, :], 0.0),
        axis=2,
    )
    picked_exp = jnp.exp(picked)
    pair_share = picked_exp / jnp.sum(picked_exp, axis=1, keepdims=True)
    group_of = chosen // (expert_count // group_count)
    group_ids = jnp.arange(group_count, dtype=jnp.int32)
    group_share = jnp.sum(
        jnp.where(group_of[:, :, None] == group_ids[None, None, :], group_prob[:, None, :], 0.0),
        axis=2,
    )
    return group_share * pair_share


def expert_ffn(arrived, expert_gate, expert_up, expert_down):
    sources, slot_count, width = arrived.shape
    gathered = arrived.reshape(sources * slot_count, width)
    gate_out = jnp.dot(gathered, expert_gate[0], preferred_element_type=jnp.float32)
    up_out = jnp.dot(gathered, expert_up[0], preferred_element_type=jnp.float32)
    hidden = (jax.nn.silu(gate_out) * up_out).astype(jnp.bfloat16)
    result = jnp.dot(hidden, expert_down[0], preferred_element_type=jnp.float32).astype(
        jnp.bfloat16
    )
    return result.reshape(sources, slot_count, width)


def fill_slots(normed, chosen, capacity, expert_count):
    flat_routes = chosen.reshape(-1)
    entry_count = flat_routes.shape[0]
    onehot = (flat_routes[:, None] == jnp.arange(expert_count, dtype=jnp.int32)[None, :]).astype(
        jnp.int32
    )
    slot_rank = jnp.sum((jnp.cumsum(onehot, axis=0) - onehot) * onehot, axis=1)
    slot_index = flat_routes * capacity + slot_rank
    token_ids = jnp.arange(entry_count, dtype=jnp.int32) // chosen.shape[1]
    source_row = (
        jnp.full((expert_count * capacity,), normed.shape[0], jnp.int32)
        .at[slot_index]
        .set(token_ids)
    )
    padded = jnp.concatenate([normed, jnp.zeros((1, normed.shape[1]), normed.dtype)], axis=0)
    outgoing = jnp.take(padded, source_row, axis=0).reshape(expert_count, capacity, normed.shape[1])
    return (outgoing, slot_index)


def combine_rows(returned, slot_index, weight):
    flat_out = returned.reshape(-1, returned.shape[2])
    picked = jnp.take(flat_out, slot_index, axis=0).reshape(
        weight.shape[0], weight.shape[1], flat_out.shape[1]
    )
    return jnp.sum(weight[:, :, None] * picked.astype(jnp.float32), axis=1)


MESH = pl.DeviceIdType.MESH
group_size = 4


def flip(index, bit):
    return index + bit - 2 * bit * ((index // bit) % 2)


def experts_kernel(
    dims,
    residual,
    pool_input,
    docs,
    pool_map,
    pool_scale,
    out_weight,
    mix_gain,
    mix_shift,
    routers,
    chosen,
    own_gate,
    own_up,
    own_down,
    gain,
    shift,
    out,
    tail,
    tail_docs,
    mapped,
    mixed_in,
    projection,
    values_in,
    normed,
    meta,
    gate_a,
    up_a,
    down_a,
    gate_b,
    up_b,
    down_b,
    rows_in,
    meta_in,
    picked,
    spread,
    slot_weight,
    hidden,
    weighted,
    partial,
    passing,
    arrived,
    load_sems,
    send_sems,
    recv_sems,
):
    slots, expert_count, group_count, tp_count = dims
    rows, width = normed.shape
    half = rows // 2
    ff = own_gate.shape[2]
    piece = ff // tp_count
    seq_rows, pool_width = pool_input.shape
    reach = tail.shape[0]
    sp, tp = lax.axis_index("sp"), lax.axis_index("tp")
    to_y = {"sp": flip(sp, 1)}
    to_z = {"sp": flip(sp, 2)}
    to_far = {"sp": flip(sp, group_size)}
    to_x = {"tp": flip(tp, 2)}
    to_core = {"tp": flip(tp, 1)}
    to_cross = {"tp": flip(flip(tp, 1), 2)}
    to_next = {"sp": (sp + 1) % expert_count}
    to_previous = {"sp": (sp + expert_count - 1) % expert_count}

    loads = [
        pltpu.make_async_copy(own_gate.at[0], gate_a, load_sems.at[0]),
        pltpu.make_async_copy(own_up.at[0], up_a, load_sems.at[1]),
        pltpu.make_async_copy(own_down.at[0], down_a, load_sems.at[2]),
    ]
    load_projection = pltpu.make_async_copy(out_weight, projection, load_sems.at[3])
    load_projection.start()
    for load in loads:
        load.start()

    barrier = pltpu.get_barrier_semaphore()
    peers = (to_y, to_z, to_far, to_x, to_core, to_cross, to_next, to_previous)
    for peer in peers:
        pl.semaphore_signal(barrier, inc=1, device_id=peer, device_id_type=MESH)
    pl.semaphore_wait(barrier, len(peers))

    made = []

    def send(src, dst, peer):
        index = len(made)
        copy = pltpu.make_async_remote_copy(
            src_ref=src,
            dst_ref=dst,
            send_sem=send_sems.at[index],
            recv_sem=recv_sems.at[index],
            device_id=peer,
            device_id_type=MESH,
        )
        copy.start()
        made.append(copy)
        return copy

    first, second = pl.ds(0, half), pl.ds(half, half)

    def cols(position):
        return pl.ds(pl.multiple_of(position * piece, piece), piece)

    mine, across = cols(tp), cols(flip(tp, 2))

    last = pl.ds(seq_rows - reach, reach)
    tail_copy = send(pool_input.at[last], tail, to_next)
    docs_copy = send(docs.at[last], tail_docs, to_next)
    gate_far = send(own_gate.at[0, :, mine], gate_b.at[:, mine], to_far)

    expert_rows = lax.broadcasted_iota(jnp.int32, (2 * expert_count, rows), 0)
    named = (expert_rows == chosen[0:1, :]) | (expert_rows == chosen[1:2, :])
    earlier = lax.broadcasted_iota(jnp.int32, (rows, rows), 0)
    later = lax.broadcasted_iota(jnp.int32, (rows, rows), 1)
    ahead = (earlier < later) & ((earlier < half) == (later < half))
    rank = jnp.dot(
        jnp.where(named, 1.0, 0.0).astype(jnp.bfloat16),
        jnp.where(ahead, 1.0, 0.0).astype(jnp.bfloat16),
        preferred_element_type=jnp.float32,
    )[:expert_count]
    named = named[:expert_count]
    in_second = lax.broadcasted_iota(jnp.int32, (expert_count, rows), 1) >= half
    rank = rank + jnp.where(in_second, float(slots // 2), 0.0)
    meta[:expert_count, :] = jnp.where(named, rank, -1.0)

    tail_copy.wait_recv()
    docs_copy.wait_recv()
    before_docs = jnp.where(sp == 0, -1, tail_docs[...])
    all_docs = jnp.concatenate([before_docs, docs[...]], axis=0)
    lanes = docs.shape[1]
    steps = reach.bit_length() - 1
    same = [
        (pltpu.roll(all_docs, 2**step, 0) == all_docs) & (step <= tp) for step in range(steps)
    ]
    count = jnp.ones(all_docs.shape, jnp.float32)
    for step in range(steps):
        count = count + jnp.where(same[step], pltpu.roll(count, 2**step, 0), 0.0)
    for block in range(pool_width // lanes):
        where = slice(block * lanes, (block + 1) * lanes)
        source = jnp.concatenate(
            [tail[:, where].astype(jnp.float32), pool_input[:, where].astype(jnp.float32)], axis=0
        )
        running = source
        for step in range(steps):
            running = running + jnp.where(same[step], pltpu.roll(running, 2**step, 0), 0.0)
        pooled = running / count - source
        mapped[:, where] = pooled[reach:].astype(jnp.bfloat16)

    @pl.loop(0, tp_count)
    def _(block):
        where = pl.ds(pl.multiple_of(block * rows, rows), rows)
        result = jnp.dot(mapped[where, :], pool_map[0], preferred_element_type=jnp.float32)
        mapped[where, :] = (result * pool_scale[...]).astype(jnp.bfloat16)

    def owner_rows(position):
        return pl.ds(pl.multiple_of(position * rows, rows), rows)

    mixed_copies = []
    for peer in (to_x, to_cross, to_core):
        mixed_copies.append(send(mapped.at[owner_rows(peer["tp"])], mixed_in.at[tp], peer))
    mixed_in[tp] = mapped[owner_rows(tp), :]
    load_projection.wait()
    for copy in mixed_copies:
        copy.wait_recv()

    @pl.loop(0, 4)
    def _(step):
        wide = width // 4
        block = pl.ds(pl.multiple_of(step * wide, wide), wide)
        total = skip_scale * residual[:, block].astype(jnp.float32)
        for group in range(tp_count):
            total = total + jnp.dot(
                mixed_in[group],
                projection[group * pool_width : (group + 1) * pool_width, block],
                preferred_element_type=jnp.float32,
            )
        values_in[:, block] = total

    @pl.loop(0, rows // 64)
    def _(step):
        block = pl.ds(pl.multiple_of(step * 64, 64), 64)
        normed[block, :] = layer_norm(values_in[block, :], mix_gain[...], mix_shift[...]).astype(
            jnp.bfloat16
        )

    rows_y1 = send(normed.at[first], rows_in.at[0, first], to_y)
    rows_z2 = send(normed.at[second], rows_in.at[1, second], to_z)
    rows_y2 = send(normed.at[second], rows_in.at[0, second], to_y)
    rows_z1 = send(normed.at[first], rows_in.at[1, first], to_z)

    logits = lax.dot_general(
        routers[...], normed[...], (((1,), (1,)), ((), ())), preferred_element_type=jnp.float32
    )
    group_exp = jnp.exp(logits[expert_count : expert_count + group_count])
    group_prob = group_exp / jnp.sum(group_exp, axis=0, keepdims=True)
    group_of = lax.broadcasted_iota(jnp.int32, (expert_count, rows), 0) // (
        expert_count // group_count
    )
    group_share = jnp.zeros((expert_count, rows), jnp.float32)
    for group in range(group_count):
        group_share = jnp.where(group_of == group, group_prob[group : group + 1], group_share)
    picked_exp = jnp.where(named, jnp.exp(jnp.where(named, logits[:expert_count], 0.0)), 0.0)
    pair_share = picked_exp / jnp.sum(picked_exp, axis=0, keepdims=True)
    meta[expert_count:, :] = group_share * pair_share
    meta_y = send(meta, meta_in.at[0], to_y)
    meta_z = send(meta, meta_in.at[1], to_z)

    slot_ids = lax.broadcasted_iota(jnp.int32, (slots, rows), 0).astype(jnp.float32)
    experts = (sp, flip(sp, group_size))

    def select(position, row_ref, meta_ref):
        parts = []
        for which in range(2):
            slot_row = meta_ref[pl.ds(experts[which], 1), :]
            weight_row = meta_ref[pl.ds(expert_count + experts[which], 1), :]
            match = jnp.where(slot_ids == slot_row, 1.0, 0.0)
            slot_weight[position, pl.ds(which * slots, slots), :] = jnp.sum(
                match * weight_row, axis=1, keepdims=True
            )
            parts.append(match)
        match = jnp.concatenate(parts, axis=0)
        spread[position] = jnp.transpose(match).astype(jnp.bfloat16)
        match = match.astype(jnp.bfloat16)

        @pl.loop(0, 4)
        def _(step):
            wide = width // 4
            block = pl.ds(pl.multiple_of(step * wide, wide), wide)
            picked[position, :, block] = jnp.dot(
                match, row_ref[:, block], preferred_element_type=jnp.float32
            ).astype(jnp.bfloat16)

    def ffn(position, which, gate, up, down):
        where = pl.ds(which * slots, slots)

        @pl.loop(0, 2)
        def _(step):
            wide = ff // 2
            block = pl.ds(pl.multiple_of(step * wide, wide), wide)
            values = picked[position, where, :]
            gate_out = jnp.dot(values, gate[:, block], preferred_element_type=jnp.float32)
            up_out = jnp.dot(values, up[:, block], preferred_element_type=jnp.float32)
            hidden[:, block] = (gate_out / (1.0 + jnp.exp(-gate_out)) * up_out).astype(
                jnp.bfloat16
            )

        @pl.loop(0, 4)
        def _(step):
            wide = width // 4
            block = pl.ds(pl.multiple_of(step * wide, wide), wide)
            result = jnp.dot(hidden[...], down[:, block], preferred_element_type=jnp.float32)
            weighted[position, where, block] = (
                result * slot_weight[position, where, :]
            ).astype(jnp.bfloat16)

    def gather_back(position):
        @pl.loop(0, 4)
        def _(step):
            wide = width // 4
            block = pl.ds(pl.multiple_of(step * wide, wide), wide)
            partial[position, :, block] = jnp.dot(
                spread[position], weighted[position, :, block], preferred_element_type=jnp.float32
            ).astype(jnp.bfloat16)

    own, from_y, from_z, from_corner = 3, 0, 1, 2
    gate_far.wait_recv()
    gate_x = send(gate_b.at[:, mine], gate_b.at[:, mine], to_x)
    gate_c = send(gate_b.at[:, mine], gate_b.at[:, mine], to_core)
    select(own, normed, meta)
    for load in loads:
        load.wait()
    ffn(own, 0, gate_a, up_a, down_a)

    rows_y1.wait_recv()
    rows_corner1 = send(rows_in.at[0, first], rows_in.at[2, first], to_z)
    meta_y.wait_recv()
    meta_corner = send(meta_in.at[0], meta_in.at[2], to_z)
    up_far = send(own_up.at[0, :, mine], up_b.at[:, mine], to_far)
    down_far = send(own_down.at[0, mine], down_b.at[mine], to_far)
    rows_z2.wait_recv()
    rows_corner2 = send(rows_in.at[1, second], rows_in.at[2, second], to_y)
    gate_x.wait_recv()
    gate_relay = send(gate_b.at[:, across], gate_b.at[:, across], to_core)

    rows_y2.wait_recv()
    select(from_y, rows_in.at[0], meta_in.at[0])
    ffn(from_y, 0, gate_a, up_a, down_a)
    meta_z.wait_recv()
    rows_z1.wait_recv()
    select(from_z, rows_in.at[1], meta_in.at[1])
    ffn(from_z, 0, gate_a, up_a, down_a)
    up_far.wait_recv()
    up_x = send(up_b.at[:, mine], up_b.at[:, mine], to_x)
    up_c = send(up_b.at[:, mine], up_b.at[:, mine], to_core)
    meta_corner.wait_recv()
    rows_corner1.wait_recv()
    rows_corner2.wait_recv()
    select(from_corner, rows_in.at[2], meta_in.at[2])
    ffn(from_corner, 0, gate_a, up_a, down_a)
    down_far.wait_recv()
    down_x = send(down_b.at[mine], down_b.at[mine], to_x)
    down_c = send(down_b.at[mine], down_b.at[mine], to_core)
    up_x.wait_recv()
    up_relay = send(up_b.at[:, across], up_b.at[:, across], to_core)
    down_x.wait_recv()
    down_relay = send(down_b.at[across], down_b.at[across], to_core)
    for copy in (gate_c, up_c, gate_relay, up_relay, down_c, down_relay):
        copy.wait_recv()

    ffn(from_corner, 1, gate_b, up_b, down_b)
    gather_back(from_corner)
    pass_y = send(partial.at[from_corner, first], passing.at[0], to_y)
    pass_z = send(partial.at[from_corner, second], passing.at[1], to_z)
    ffn(from_y, 1, gate_b, up_b, down_b)
    gather_back(from_y)
    back_y1 = send(partial.at[from_y, first], arrived.at[0, first], to_y)
    ffn(from_z, 1, gate_b, up_b, down_b)
    gather_back(from_z)
    back_z2 = send(partial.at[from_z, second], arrived.at[1, second], to_z)

    def add_passing(position, where, slot):
        partial[position, where, :] = (
            partial[position, where, :].astype(jnp.float32) + passing[slot].astype(jnp.float32)
        ).astype(jnp.bfloat16)

    pass_y.wait_recv()
    add_passing(from_z, first, 0)
    back_z1 = send(partial.at[from_z, first], arrived.at[1, first], to_z)
    pass_z.wait_recv()
    add_passing(from_y, second, 1)
    back_y2 = send(partial.at[from_y, second], arrived.at[0, second], to_y)
    ffn(own, 1, gate_b, up_b, down_b)
    for copy in (back_y1, back_z2, back_z1, back_y2):
        copy.wait_recv()

    @pl.loop(0, rows // 64)
    def _(step):
        block = pl.ds(pl.multiple_of(step * 64, 64), 64)
        routed = jnp.dot(spread[own, block, :], weighted[own], preferred_element_type=jnp.float32)
        routed = routed + arrived[0, block, :].astype(jnp.float32)
        routed = routed + arrived[1, block, :].astype(jnp.float32)
        values = skip_scale * normed[block, :].astype(jnp.float32) + routed
        out[block, :] = layer_norm(values, gain[...], shift[...]).astype(jnp.bfloat16)

    for copy in made:
        copy.wait_send()


def whole_layer(
    residual,
    pool_input,
    doc_ids,
    pool_map,
    pool_scale,
    out_weight,
    mix_gain,
    mix_shift,
    group_router,
    expert_router,
    expert_gate,
    expert_up,
    expert_down,
    routes,
    ffn_gain,
    ffn_shift,
):
    expert_count, tp_count = lax.axis_size("sp"), lax.axis_size("tp")
    rows, width = residual.shape
    ff = expert_gate.shape[2]
    seq_rows, pool_width = pool_input.shape
    group_count = group_router.shape[1]
    slots = 2 * rows * routes.shape[1] // expert_count
    reach = 16
    lanes = 128
    docs = jnp.broadcast_to(doc_ids[:, None], (seq_rows, lanes))
    routers = jnp.concatenate([expert_router.T, group_router.T], axis=0)
    routers = jnp.pad(routers, ((0, 2 * expert_count - routers.shape[0]), (0, 0)))
    vmem = pl.BlockSpec(memory_space=pltpu.VMEM)
    anywhere = pl.BlockSpec(memory_space=pl.ANY)
    bf16, f32 = jnp.bfloat16, jnp.float32
    table = (2 * expert_count, rows)
    return pl.pallas_call(
        functools.partial(experts_kernel, (slots, expert_count, group_count, tp_count)),
        out_shape=jax.ShapeDtypeStruct((rows, width), bf16),
        in_specs=[vmem] * 5 + [anywhere] + [vmem] * 4 + [anywhere] * 3 + [vmem] * 2,
        out_specs=vmem,
        scratch_shapes=[
            pltpu.VMEM((reach, pool_width), bf16),
            pltpu.VMEM((reach, lanes), jnp.int32),
            pltpu.VMEM((seq_rows, pool_width), bf16),
            pltpu.VMEM((tp_count, rows, pool_width), bf16),
            pltpu.VMEM(out_weight.shape, bf16),
            pltpu.VMEM((rows, width), f32),
            pltpu.VMEM((rows, width), bf16),
            pltpu.VMEM(table, f32),
            pltpu.VMEM((width, ff), bf16),
            pltpu.VMEM((width, ff), bf16),
            pltpu.VMEM((ff, width), bf16),
            pltpu.VMEM((width, ff), bf16),
            pltpu.VMEM((width, ff), bf16),
            pltpu.VMEM((ff, width), bf16),
            pltpu.VMEM((3, rows, width), bf16),
            pltpu.VMEM((3,) + table, f32),
            pltpu.VMEM((4, 2 * slots, width), bf16),
            pltpu.VMEM((4, rows, 2 * slots), bf16),
            pltpu.VMEM((4, 2 * slots, 1), f32),
            pltpu.VMEM((slots, ff), bf16),
            pltpu.VMEM((4, 2 * slots, width), bf16),
            pltpu.VMEM((3, rows, width), bf16),
            pltpu.VMEM((2, rows // 2, width), bf16),
            pltpu.VMEM((2, rows, width), bf16),
            pltpu.SemaphoreType.DMA((4,)),
            pltpu.SemaphoreType.DMA((32,)),
            pltpu.SemaphoreType.DMA((32,)),
        ],
        compiler_params=pltpu.CompilerParams(
            collective_id=0, has_side_effects=True, vmem_limit_bytes=62 * 1024 * 1024
        ),
    )(
        residual,
        pool_input,
        docs,
        pool_map,
        pool_scale[None, :],
        out_weight,
        mix_gain[None, :],
        mix_shift[None, :],
        routers,
        routes.T,
        expert_gate,
        expert_up,
        expert_down,
        ffn_gain[None, :],
        ffn_shift[None, :],
    )


def on_device(
    residual,
    pool_input,
    doc_ids,
    pool_map,
    pool_scale,
    out_weight,
    mix_gain,
    mix_shift,
    group_router,
    expert_router,
    expert_gate,
    expert_up,
    expert_down,
    routes,
    ffn_gain,
    ffn_shift,
):
    seq_rows = pool_input.shape[0]
    reach_rows = 15
    expert_count = lax.axis_size("sp")
    tp_count = lax.axis_size("tp")
    if expert_count == 2 * group_size and tp_count == group_size:
        return whole_layer(
            residual,
            pool_input,
            doc_ids,
            pool_map,
            pool_scale,
            out_weight,
            mix_gain,
            mix_shift,
            group_router,
            expert_router,
            expert_gate,
            expert_up,
            expert_down,
            routes,
            ffn_gain,
            ffn_shift,
        )
    window = jnp.left_shift(jnp.int32(2), lax.axis_index("tp"))
    first_row = lax.axis_index("sp") * seq_rows
    tail_values, tail_docs = from_behind(
        (pool_input[seq_rows - reach_rows :], doc_ids[seq_rows - reach_rows :]), "sp", 1
    )
    source = jnp.concatenate([tail_values, pool_input], axis=0).astype(jnp.float32)
    all_docs = jnp.concatenate([tail_docs, doc_ids], axis=0)
    positions = first_row - reach_rows + jnp.arange(seq_rows + reach_rows, dtype=jnp.int32)
    running = jnp.zeros((seq_rows, source.shape[1]), jnp.float32)
    weight_sum = jnp.zeros((seq_rows, 1), jnp.float32)
    for offset in range(reach_rows + 1):
        begin_row = reach_rows - offset
        earlier = source[begin_row : begin_row + seq_rows]
        keep_mask = (
            (all_docs[begin_row : begin_row + seq_rows] == doc_ids)
            & (positions[begin_row : begin_row + seq_rows] >= 0)
            & (offset < window)
        )
        same_doc = keep_mask.astype(jnp.float32)[:, None]
        running = running + same_doc * earlier
        weight_sum = weight_sum + same_doc
    pooled = (running / weight_sum - source[reach_rows:]).astype(jnp.bfloat16)
    mixed = (jnp.dot(pooled, pool_map[0], preferred_element_type=jnp.float32) * pool_scale).astype(
        jnp.bfloat16
    )
    row_count = seq_rows // tp_count
    blocks = mixed.reshape(tp_count, row_count, mixed.shape[1])
    branch = jnp.einsum(
        "abc,cd->abd",
        lax.all_to_all(blocks, "tp", split_axis=0, concat_axis=2, tiled=True),
        out_weight,
        preferred_element_type=jnp.float32,
    )[0]
    normed = layer_norm(
        skip_scale * residual.astype(jnp.float32) + branch, mix_gain, mix_shift
    ).astype(jnp.bfloat16)
    weight = route_weights(normed, routes, group_router, expert_router)
    half_most = row_count * routes.shape[1] // expert_count
    half_rows = row_count // 2
    routed_parts = []
    for piece_index in range(2):
        rows_here = slice(piece_index * half_rows, (piece_index + 1) * half_rows)
        outgoing, slot_index = fill_slots(
            normed[rows_here], routes[rows_here], half_most, expert_count
        )
        returned = lax.all_to_all(
            expert_ffn(
                lax.all_to_all(outgoing, "sp", split_axis=0, concat_axis=0, tiled=True),
                expert_gate,
                expert_up,
                expert_down,
            ),
            "sp",
            split_axis=0,
            concat_axis=0,
            tiled=True,
        )
        routed_parts.append(combine_rows(returned, slot_index, weight[rows_here]))
    routed = jnp.concatenate(routed_parts, axis=0)
    return layer_norm(skip_scale * normed.astype(jnp.float32) + routed, ffn_gain, ffn_shift).astype(
        jnp.bfloat16
    )


def solution(mesh):
    in_specs = (
        P(("sp", "tp"), None),
        P("sp", "tp"),
        P("sp"),
        P("tp", None, None),
        P("tp"),
        P(),
        P(),
        P(),
        P(),
        P(),
        P("sp", None, None),
        P("sp", None, None),
        P("sp", None, None),
        P(("sp", "tp"), None),
        P(),
        P(),
    )
    out_specs = P(("sp", "tp"), None)
    return jax.shard_map(
        on_device, mesh=mesh, in_specs=in_specs, out_specs=out_specs, check_vma=False
    )
```

```python
import functools

import jax
import jax.numpy as jnp
from jax import lax
from jax.experimental import pallas as pl
from jax.experimental.pallas import tpu as pltpu
from jax.sharding import PartitionSpec as P

skip_scale = 2.0**0.5
epsilon = 1e-05


def from_behind(block, axis, distance):
    devices = range(lax.axis_size(axis))
    route = [(i - distance, i) for i in devices if i - distance in devices]
    return lax.ppermute(block, axis, route)


def layer_norm(values, norm_gain, norm_shift):
    center = values - jnp.mean(values, axis=-1, keepdims=True)
    spread = jnp.mean(center * center, axis=-1, keepdims=True)
    return center * lax.rsqrt(spread + epsilon) * norm_gain + norm_shift


def route_weights(normed, chosen, group_router, expert_router):
    group_logits = jnp.dot(normed, group_router, preferred_element_type=jnp.float32)
    expert_logits = jnp.dot(normed, expert_router, preferred_element_type=jnp.float32)
    group_count = group_logits.shape[1]
    expert_count = expert_logits.shape[1]
    group_exp = jnp.exp(group_logits)
    group_prob = group_exp / jnp.sum(group_exp, axis=1, keepdims=True)
    expert_ids = jnp.arange(expert_count, dtype=jnp.int32)
    picked = jnp.sum(
        jnp.where(chosen[:, :, None] == expert_ids[None, None, :], expert_logits[:, None, :], 0.0),
        axis=2,
    )
    picked_exp = jnp.exp(picked)
    pair_share = picked_exp / jnp.sum(picked_exp, axis=1, keepdims=True)
    group_of = chosen // (expert_count // group_count)
    group_ids = jnp.arange(group_count, dtype=jnp.int32)
    group_share = jnp.sum(
        jnp.where(group_of[:, :, None] == group_ids[None, None, :], group_prob[:, None, :], 0.0),
        axis=2,
    )
    return group_share * pair_share


def expert_ffn(arrived, expert_gate, expert_up, expert_down):
    sources, slot_count, width = arrived.shape
    gathered = arrived.reshape(sources * slot_count, width)
    gate_out = jnp.dot(gathered, expert_gate[0], preferred_element_type=jnp.float32)
    up_out = jnp.dot(gathered, expert_up[0], preferred_element_type=jnp.float32)
    hidden = (jax.nn.silu(gate_out) * up_out).astype(jnp.bfloat16)
    result = jnp.dot(hidden, expert_down[0], preferred_element_type=jnp.float32).astype(
        jnp.bfloat16
    )
    return result.reshape(sources, slot_count, width)


def fill_slots(normed, chosen, capacity, expert_count):
    flat_routes = chosen.reshape(-1)
    entry_count = flat_routes.shape[0]
    onehot = (flat_routes[:, None] == jnp.arange(expert_count, dtype=jnp.int32)[None, :]).astype(
        jnp.int32
    )
    slot_rank = jnp.sum((jnp.cumsum(onehot, axis=0) - onehot) * onehot, axis=1)
    slot_index = flat_routes * capacity + slot_rank
    token_ids = jnp.arange(entry_count, dtype=jnp.int32) // chosen.shape[1]
    source_row = (
        jnp.full((expert_count * capacity,), normed.shape[0], jnp.int32)
        .at[slot_index]
        .set(token_ids)
    )
    padded = jnp.concatenate([normed, jnp.zeros((1, normed.shape[1]), normed.dtype)], axis=0)
    outgoing = jnp.take(padded, source_row, axis=0).reshape(expert_count, capacity, normed.shape[1])
    return (outgoing, slot_index)


def combine_rows(returned, slot_index, weight):
    flat_out = returned.reshape(-1, returned.shape[2])
    picked = jnp.take(flat_out, slot_index, axis=0).reshape(
        weight.shape[0], weight.shape[1], flat_out.shape[1]
    )
    return jnp.sum(weight[:, :, None] * picked.astype(jnp.float32), axis=1)


MESH = pl.DeviceIdType.MESH
group_size = 4


def flip(index, bit):
    return index + bit - 2 * bit * ((index // bit) % 2)


def experts_kernel(
    dims,
    residual,
    pool_input,
    docs,
    pool_map,
    pool_scale,
    out_weight,
    mix_gain,
    mix_shift,
    routers,
    chosen,
    own_gate,
    own_up,
    own_down,
    gain,
    shift,
    out,
    tail,
    tail_docs,
    mapped,
    mixed_in,
    projection,
    values_in,
    normed,
    meta,
    gate_a,
    up_a,
    down_a,
    gate_b,
    up_b,
    down_b,
    rows_in,
    meta_in,
    picked,
    spread,
    slot_weight,
    hidden,
    weighted,
    partial,
    passing,
    arrived,
    load_sems,
    send_sems,
    recv_sems,
):
    slots, expert_count, group_count, tp_count = dims
    rows, width = normed.shape
    half = rows // 2
    ff = own_gate.shape[2]
    piece = ff // tp_count
    seq_rows, pool_width = pool_input.shape
    reach = tail.shape[0]
    sp, tp = lax.axis_index("sp"), lax.axis_index("tp")
    to_y = {"sp": flip(sp, 1)}
    to_z = {"sp": flip(sp, 2)}
    to_far = {"sp": flip(sp, group_size)}
    to_x = {"tp": flip(tp, 2)}
    to_core = {"tp": flip(tp, 1)}
    to_cross = {"tp": flip(flip(tp, 1), 2)}
    to_next = {"sp": (sp + 1) % expert_count}
    to_previous = {"sp": (sp + expert_count - 1) % expert_count}

    loads = [
        pltpu.make_async_copy(own_gate.at[0], gate_a, load_sems.at[0]),
        pltpu.make_async_copy(own_up.at[0], up_a, load_sems.at[1]),
        pltpu.make_async_copy(own_down.at[0], down_a, load_sems.at[2]),
    ]
    load_projection = pltpu.make_async_copy(out_weight, projection, load_sems.at[3])
    load_projection.start()
    for load in loads:
        load.start()

    barrier = pltpu.get_barrier_semaphore()
    peers = (to_y, to_z, to_far, to_x, to_core, to_cross, to_next, to_previous)
    for peer in peers:
        pl.semaphore_signal(barrier, inc=1, device_id=peer, device_id_type=MESH)
    pl.semaphore_wait(barrier, len(peers))

    made = []

    def send(src, dst, peer):
        index = len(made)
        copy = pltpu.make_async_remote_copy(
            src_ref=src,
            dst_ref=dst,
            send_sem=send_sems.at[index],
            recv_sem=recv_sems.at[index],
            device_id=peer,
            device_id_type=MESH,
        )
        copy.start()
        made.append(copy)
        return copy

    first, second = pl.ds(0, half), pl.ds(half, half)

    def cols(position):
        return pl.ds(pl.multiple_of(position * piece, piece), piece)

    def deep(position):
        size = width // tp_count
        return pl.ds(pl.multiple_of(position * size, size), size)

    mine, across = cols(tp), cols(flip(tp, 2))
    deep_mine, deep_across = deep(tp), deep(flip(tp, 2))

    last = pl.ds(seq_rows - reach, reach)
    tail_copy = send(pool_input.at[last], tail, to_next)
    docs_copy = send(docs.at[last], tail_docs, to_next)
    gate_far = send(own_gate.at[0, deep_mine], gate_b.at[deep_mine], to_far)
    up_far = send(own_up.at[0, deep_mine], up_b.at[deep_mine], to_far)

    expert_rows = lax.broadcasted_iota(jnp.int32, (2 * expert_count, rows), 0)
    named = (expert_rows == chosen[0:1, :]) | (expert_rows == chosen[1:2, :])
    earlier = lax.broadcasted_iota(jnp.int32, (rows, rows), 0)
    later = lax.broadcasted_iota(jnp.int32, (rows, rows), 1)
    ahead = (earlier < later) & ((earlier < half) == (later < half))
    rank = jnp.dot(
        jnp.where(named, 1.0, 0.0).astype(jnp.bfloat16),
        jnp.where(ahead, 1.0, 0.0).astype(jnp.bfloat16),
        preferred_element_type=jnp.float32,
    )[:expert_count]
    named = named[:expert_count]
    in_second = lax.broadcasted_iota(jnp.int32, (expert_count, rows), 1) >= half
    rank = rank + jnp.where(in_second, float(slots // 2), 0.0)
    meta[:expert_count, :] = jnp.where(named, rank, -1.0)

    tail_copy.wait_recv()
    docs_copy.wait_recv()
    before_docs = jnp.where(sp == 0, -1, tail_docs[...])
    all_docs = jnp.concatenate([before_docs, docs[...]], axis=0)
    lanes = docs.shape[1]
    steps = reach.bit_length() - 1
    same = [
        (pltpu.roll(all_docs, 2**step, 0) == all_docs) & (step <= tp) for step in range(steps)
    ]
    count = jnp.ones(all_docs.shape, jnp.float32)
    for step in range(steps):
        count = count + jnp.where(same[step], pltpu.roll(count, 2**step, 0), 0.0)
    for block in range(pool_width // lanes):
        where = slice(block * lanes, (block + 1) * lanes)
        source = jnp.concatenate(
            [tail[:, where].astype(jnp.float32), pool_input[:, where].astype(jnp.float32)], axis=0
        )
        running = source
        for step in range(steps):
            running = running + jnp.where(same[step], pltpu.roll(running, 2**step, 0), 0.0)
        pooled = running / count - source
        mapped[:, where] = pooled[reach:].astype(jnp.bfloat16)

    @pl.loop(0, tp_count)
    def _(block):
        where = pl.ds(pl.multiple_of(block * rows, rows), rows)
        result = jnp.dot(mapped[where, :], pool_map[0], preferred_element_type=jnp.float32)
        mapped[where, :] = (result * pool_scale[...]).astype(jnp.bfloat16)

    def owner_rows(position):
        return pl.ds(pl.multiple_of(position * rows, rows), rows)

    mixed_copies = []
    for peer in (to_x, to_cross, to_core):
        mixed_copies.append(send(mapped.at[owner_rows(peer["tp"])], mixed_in.at[tp], peer))
    mixed_in[tp] = mapped[owner_rows(tp), :]
    load_projection.wait()
    for copy in mixed_copies:
        copy.wait_recv()

    @pl.loop(0, 4)
    def _(step):
        wide = width // 4
        block = pl.ds(pl.multiple_of(step * wide, wide), wide)
        total = skip_scale * residual[:, block].astype(jnp.float32)
        for group in range(tp_count):
            total = total + jnp.dot(
                mixed_in[group],
                projection[group * pool_width : (group + 1) * pool_width, block],
                preferred_element_type=jnp.float32,
            )
        values_in[:, block] = total

    @pl.loop(0, rows // 64)
    def _(step):
        block = pl.ds(pl.multiple_of(step * 64, 64), 64)
        normed[block, :] = layer_norm(values_in[block, :], mix_gain[...], mix_shift[...]).astype(
            jnp.bfloat16
        )

    rows_y1 = send(normed.at[first], rows_in.at[0, first], to_y)
    rows_z2 = send(normed.at[second], rows_in.at[1, second], to_z)
    rows_y2 = send(normed.at[second], rows_in.at[0, second], to_y)
    rows_z1 = send(normed.at[first], rows_in.at[1, first], to_z)

    logits = lax.dot_general(
        routers[...], normed[...], (((1,), (1,)), ((), ())), preferred_element_type=jnp.float32
    )
    group_exp = jnp.exp(logits[expert_count : expert_count + group_count])
    group_prob = group_exp / jnp.sum(group_exp, axis=0, keepdims=True)
    group_of = lax.broadcasted_iota(jnp.int32, (expert_count, rows), 0) // (
        expert_count // group_count
    )
    group_share = jnp.zeros((expert_count, rows), jnp.float32)
    for group in range(group_count):
        group_share = jnp.where(group_of == group, group_prob[group : group + 1], group_share)
    picked_exp = jnp.where(named, jnp.exp(jnp.where(named, logits[:expert_count], 0.0)), 0.0)
    pair_share = picked_exp / jnp.sum(picked_exp, axis=0, keepdims=True)
    meta[expert_count:, :] = group_share * pair_share
    meta_y = send(meta, meta_in.at[0], to_y)
    meta_z = send(meta, meta_in.at[1], to_z)
    down_far = send(own_down.at[0, mine], down_b.at[mine], to_far)

    slot_ids = lax.broadcasted_iota(jnp.int32, (slots, rows), 0).astype(jnp.float32)
    experts = (sp, flip(sp, group_size))

    def select(position, row_ref, meta_ref):
        parts = []
        for which in range(2):
            slot_row = meta_ref[pl.ds(experts[which], 1), :]
            weight_row = meta_ref[pl.ds(expert_count + experts[which], 1), :]
            match = jnp.where(slot_ids == slot_row, 1.0, 0.0)
            slot_weight[position, pl.ds(which * slots, slots), :] = jnp.sum(
                match * weight_row, axis=1, keepdims=True
            )
            parts.append(match)
        match = jnp.concatenate(parts, axis=0)
        spread[position] = jnp.transpose(match).astype(jnp.bfloat16)
        match = match.astype(jnp.bfloat16)

        @pl.loop(0, 4)
        def _(step):
            wide = width // 4
            block = pl.ds(pl.multiple_of(step * wide, wide), wide)
            picked[position, :, block] = jnp.dot(
                match, row_ref[:, block], preferred_element_type=jnp.float32
            ).astype(jnp.bfloat16)

    def ffn(position, which, gate, up, down):
        where = pl.ds(which * slots, slots)

        @pl.loop(0, 2)
        def _(step):
            wide = ff // 2
            block = pl.ds(pl.multiple_of(step * wide, wide), wide)
            values = picked[position, where, :]
            gate_out = jnp.dot(values, gate[:, block], preferred_element_type=jnp.float32)
            up_out = jnp.dot(values, up[:, block], preferred_element_type=jnp.float32)
            hidden[:, block] = (gate_out / (1.0 + jnp.exp(-gate_out)) * up_out).astype(
                jnp.bfloat16
            )

        @pl.loop(0, 4)
        def _(step):
            wide = width // 4
            block = pl.ds(pl.multiple_of(step * wide, wide), wide)
            result = jnp.dot(hidden[...], down[:, block], preferred_element_type=jnp.float32)
            weighted[position, where, block] = (
                result * slot_weight[position, where, :]
            ).astype(jnp.bfloat16)

    def gather_back(position):
        @pl.loop(0, 4)
        def _(step):
            wide = width // 4
            block = pl.ds(pl.multiple_of(step * wide, wide), wide)
            partial[position, :, block] = jnp.dot(
                spread[position], weighted[position, :, block], preferred_element_type=jnp.float32
            ).astype(jnp.bfloat16)

    own, from_y, from_z, from_corner = 3, 0, 1, 2
    gate_far.wait_recv()
    gate_x = send(gate_b.at[deep_mine], gate_b.at[deep_mine], to_x)
    gate_c = send(gate_b.at[deep_mine], gate_b.at[deep_mine], to_core)
    select(own, normed, meta)
    for load in loads:
        load.wait()
    ffn(own, 0, gate_a, up_a, down_a)

    rows_y1.wait_recv()
    meta_y.wait_recv()
    rows_z2.wait_recv()
    rows_corner2 = send(rows_in.at[1, second], rows_in.at[2, second], to_y)
    gate_x.wait_recv()
    gate_relay = send(gate_b.at[deep_across], gate_b.at[deep_across], to_core)

    rows_y2.wait_recv()
    select(from_y, rows_in.at[0], meta_in.at[0])
    ffn(from_y, 0, gate_a, up_a, down_a)
    meta_z.wait_recv()
    meta_corner = send(meta_in.at[1], meta_in.at[2], to_y)
    rows_z1.wait_recv()
    rows_corner1 = send(rows_in.at[1, first], rows_in.at[2, first], to_y)
    select(from_z, rows_in.at[1], meta_in.at[1])
    ffn(from_z, 0, gate_a, up_a, down_a)
    up_far.wait_recv()
    up_x = send(up_b.at[deep_mine], up_b.at[deep_mine], to_x)
    up_c = send(up_b.at[deep_mine], up_b.at[deep_mine], to_core)
    meta_corner.wait_recv()
    rows_corner1.wait_recv()
    rows_corner2.wait_recv()
    select(from_corner, rows_in.at[2], meta_in.at[2])
    ffn(from_corner, 0, gate_a, up_a, down_a)
    down_far.wait_recv()
    down_x = send(down_b.at[mine], down_b.at[mine], to_x)
    down_c = send(down_b.at[mine], down_b.at[mine], to_core)
    up_x.wait_recv()
    up_relay = send(up_b.at[deep_across], up_b.at[deep_across], to_core)
    down_x.wait_recv()
    down_relay = send(down_b.at[across], down_b.at[across], to_core)
    for copy in (gate_c, up_c, gate_relay, up_relay, down_c, down_relay):
        copy.wait_recv()

    ffn(from_corner, 1, gate_b, up_b, down_b)
    gather_back(from_corner)
    pass_y = send(partial.at[from_corner, first], passing.at[0], to_y)
    pass_z = send(partial.at[from_corner, second], passing.at[1], to_z)
    ffn(from_y, 1, gate_b, up_b, down_b)
    gather_back(from_y)
    back_y1 = send(partial.at[from_y, first], arrived.at[0, first], to_y)
    ffn(from_z, 1, gate_b, up_b, down_b)
    gather_back(from_z)
    back_z2 = send(partial.at[from_z, second], arrived.at[1, second], to_z)

    def add_passing(position, where, slot):
        partial[position, where, :] = (
            partial[position, where, :].astype(jnp.float32) + passing[slot].astype(jnp.float32)
        ).astype(jnp.bfloat16)

    pass_y.wait_recv()
    add_passing(from_z, first, 0)
    back_z1 = send(partial.at[from_z, first], arrived.at[1, first], to_z)
    pass_z.wait_recv()
    add_passing(from_y, second, 1)
    back_y2 = send(partial.at[from_y, second], arrived.at[0, second], to_y)
    ffn(own, 1, gate_b, up_b, down_b)
    for copy in (back_y1, back_z2, back_z1, back_y2):
        copy.wait_recv()

    @pl.loop(0, rows // 64)
    def _(step):
        block = pl.ds(pl.multiple_of(step * 64, 64), 64)
        routed = jnp.dot(spread[own, block, :], weighted[own], preferred_element_type=jnp.float32)
        routed = routed + arrived[0, block, :].astype(jnp.float32)
        routed = routed + arrived[1, block, :].astype(jnp.float32)
        values = skip_scale * normed[block, :].astype(jnp.float32) + routed
        out[block, :] = layer_norm(values, gain[...], shift[...]).astype(jnp.bfloat16)

    for copy in made:
        copy.wait_send()


def whole_layer(
    residual,
    pool_input,
    doc_ids,
    pool_map,
    pool_scale,
    out_weight,
    mix_gain,
    mix_shift,
    group_router,
    expert_router,
    expert_gate,
    expert_up,
    expert_down,
    routes,
    ffn_gain,
    ffn_shift,
):
    expert_count, tp_count = lax.axis_size("sp"), lax.axis_size("tp")
    rows, width = residual.shape
    ff = expert_gate.shape[2]
    seq_rows, pool_width = pool_input.shape
    group_count = group_router.shape[1]
    slots = 2 * rows * routes.shape[1] // expert_count
    reach = 16
    lanes = 128
    docs = jnp.broadcast_to(doc_ids[:, None], (seq_rows, lanes))
    routers = jnp.concatenate([expert_router.T, group_router.T], axis=0)
    routers = jnp.pad(routers, ((0, 2 * expert_count - routers.shape[0]), (0, 0)))
    vmem = pl.BlockSpec(memory_space=pltpu.VMEM)
    anywhere = pl.BlockSpec(memory_space=pl.ANY)
    bf16, f32 = jnp.bfloat16, jnp.float32
    table = (2 * expert_count, rows)
    return pl.pallas_call(
        functools.partial(experts_kernel, (slots, expert_count, group_count, tp_count)),
        out_shape=jax.ShapeDtypeStruct((rows, width), bf16),
        in_specs=[vmem] * 5 + [anywhere] + [vmem] * 4 + [anywhere] * 3 + [vmem] * 2,
        out_specs=vmem,
        scratch_shapes=[
            pltpu.VMEM((reach, pool_width), bf16),
            pltpu.VMEM((reach, lanes), jnp.int32),
            pltpu.VMEM((seq_rows, pool_width), bf16),
            pltpu.VMEM((tp_count, rows, pool_width), bf16),
            pltpu.VMEM(out_weight.shape, bf16),
            pltpu.VMEM((rows, width), f32),
            pltpu.VMEM((rows, width), bf16),
            pltpu.VMEM(table, f32),
            pltpu.VMEM((width, ff), bf16),
            pltpu.VMEM((width, ff), bf16),
            pltpu.VMEM((ff, width), bf16),
            pltpu.VMEM((width, ff), bf16),
            pltpu.VMEM((width, ff), bf16),
            pltpu.VMEM((ff, width), bf16),
            pltpu.VMEM((3, rows, width), bf16),
            pltpu.VMEM((3,) + table, f32),
            pltpu.VMEM((4, 2 * slots, width), bf16),
            pltpu.VMEM((4, rows, 2 * slots), bf16),
            pltpu.VMEM((4, 2 * slots, 1), f32),
            pltpu.VMEM((slots, ff), bf16),
            pltpu.VMEM((4, 2 * slots, width), bf16),
            pltpu.VMEM((3, rows, width), bf16),
            pltpu.VMEM((2, rows // 2, width), bf16),
            pltpu.VMEM((2, rows, width), bf16),
            pltpu.SemaphoreType.DMA((4,)),
            pltpu.SemaphoreType.DMA((32,)),
            pltpu.SemaphoreType.DMA((32,)),
        ],
        compiler_params=pltpu.CompilerParams(
            collective_id=0, has_side_effects=True, vmem_limit_bytes=62 * 1024 * 1024
        ),
    )(
        residual,
        pool_input,
        docs,
        pool_map,
        pool_scale[None, :],
        out_weight,
        mix_gain[None, :],
        mix_shift[None, :],
        routers,
        routes.T,
        expert_gate,
        expert_up,
        expert_down,
        ffn_gain[None, :],
        ffn_shift[None, :],
    )


def on_device(
    residual,
    pool_input,
    doc_ids,
    pool_map,
    pool_scale,
    out_weight,
    mix_gain,
    mix_shift,
    group_router,
    expert_router,
    expert_gate,
    expert_up,
    expert_down,
    routes,
    ffn_gain,
    ffn_shift,
):
    seq_rows = pool_input.shape[0]
    reach_rows = 15
    expert_count = lax.axis_size("sp")
    tp_count = lax.axis_size("tp")
    if expert_count == 2 * group_size and tp_count == group_size:
        return whole_layer(
            residual,
            pool_input,
            doc_ids,
            pool_map,
            pool_scale,
            out_weight,
            mix_gain,
            mix_shift,
            group_router,
            expert_router,
            expert_gate,
            expert_up,
            expert_down,
            routes,
            ffn_gain,
            ffn_shift,
        )
    window = jnp.left_shift(jnp.int32(2), lax.axis_index("tp"))
    first_row = lax.axis_index("sp") * seq_rows
    tail_values, tail_docs = from_behind(
        (pool_input[seq_rows - reach_rows :], doc_ids[seq_rows - reach_rows :]), "sp", 1
    )
    source = jnp.concatenate([tail_values, pool_input], axis=0).astype(jnp.float32)
    all_docs = jnp.concatenate([tail_docs, doc_ids], axis=0)
    positions = first_row - reach_rows + jnp.arange(seq_rows + reach_rows, dtype=jnp.int32)
    running = jnp.zeros((seq_rows, source.shape[1]), jnp.float32)
    weight_sum = jnp.zeros((seq_rows, 1), jnp.float32)
    for offset in range(reach_rows + 1):
        begin_row = reach_rows - offset
        earlier = source[begin_row : begin_row + seq_rows]
        keep_mask = (
            (all_docs[begin_row : begin_row + seq_rows] == doc_ids)
            & (positions[begin_row : begin_row + seq_rows] >= 0)
            & (offset < window)
        )
        same_doc = keep_mask.astype(jnp.float32)[:, None]
        running = running + same_doc * earlier
        weight_sum = weight_sum + same_doc
    pooled = (running / weight_sum - source[reach_rows:]).astype(jnp.bfloat16)
    mixed = (jnp.dot(pooled, pool_map[0], preferred_element_type=jnp.float32) * pool_scale).astype(
        jnp.bfloat16
    )
    row_count = seq_rows // tp_count
    blocks = mixed.reshape(tp_count, row_count, mixed.shape[1])
    branch = jnp.einsum(
        "abc,cd->abd",
        lax.all_to_all(blocks, "tp", split_axis=0, concat_axis=2, tiled=True),
        out_weight,
        preferred_element_type=jnp.float32,
    )[0]
    normed = layer_norm(
        skip_scale * residual.astype(jnp.float32) + branch, mix_gain, mix_shift
    ).astype(jnp.bfloat16)
    weight = route_weights(normed, routes, group_router, expert_router)
    half_most = row_count * routes.shape[1] // expert_count
    half_rows = row_count // 2
    routed_parts = []
    for piece_index in range(2):
        rows_here = slice(piece_index * half_rows, (piece_index + 1) * half_rows)
        outgoing, slot_index = fill_slots(
            normed[rows_here], routes[rows_here], half_most, expert_count
        )
        returned = lax.all_to_all(
            expert_ffn(
                lax.all_to_all(outgoing, "sp", split_axis=0, concat_axis=0, tiled=True),
                expert_gate,
                expert_up,
                expert_down,
            ),
            "sp",
            split_axis=0,
            concat_axis=0,
            tiled=True,
        )
        routed_parts.append(combine_rows(returned, slot_index, weight[rows_here]))
    routed = jnp.concatenate(routed_parts, axis=0)
    return layer_norm(skip_scale * normed.astype(jnp.float32) + routed, ffn_gain, ffn_shift).astype(
        jnp.bfloat16
    )


def solution(mesh):
    in_specs = (
        P(("sp", "tp"), None),
        P("sp", "tp"),
        P("sp"),
        P("tp", None, None),
        P("tp"),
        P(),
        P(),
        P(),
        P(),
        P(),
        P("sp", None, None),
        P("sp", None, None),
        P("sp", None, None),
        P(("sp", "tp"), None),
        P(),
        P(),
    )
    out_specs = P(("sp", "tp"), None)
    return jax.shard_map(
        on_device, mesh=mesh, in_specs=in_specs, out_specs=out_specs, check_vma=False
    )
```
